32 devices in a mesh: sp: 4 (over z), fs: 4 (over y, x), tp: 2 (over core).
Axes of the slice: x: 2, y: 2, z: 4, core: 2. Of those that a mesh axis runs over, the one named last changes fastest.
Arguments:
- tokens: bfloat16 [4, 1024, 2048], P('fs', ('sp', 'tp')), may hold values from -6 to 6
- norm_gain: float32 [2048], replicated, may hold values from 0.1 to 1.9
- w_conv_gate: bfloat16 [2048, 1024], P('sp', 'tp'), may hold values from -0.125 to 0.125
- w_conv_in: bfloat16 [2048, 1024], P('sp', 'tp'), may hold values from -0.125 to 0.125
- w_conv_value: bfloat16 [2048, 1024], P('sp', 'tp'), may hold values from -0.125 to 0.125
- conv_taps: float32 [3, 1024], P(None, 'tp'), may hold values from -3.5 to 3.5
- w_receptance: bfloat16 [2048, 1024], P('sp', 'tp'), may hold values from -0.125 to 0.125
- w_key: bfloat16 [2048, 1024], P('sp', 'tp'), may hold values from -0.125 to 0.125
- w_value: bfloat16 [2048, 1024], P('sp', 'tp'), may hold values from -0.125 to 0.125
- w_decay_down: bfloat16 [2048, 128], P('sp'), may hold values from -0.125 to 0.125
- w_decay_up: bfloat16 [128, 1024], P(None, 'tp'), may hold values from -0.75 to 0.75
- decay_base: float32 [1024], P('tp'), may hold values from -12.5 to -3
- decay_shift: float32 [4, 1024, 1024], P('fs', 'sp', 'tp'), may hold values from -2.1 to 0
- w_rate_down: bfloat16 [2048, 128], P('sp'), may hold values from -0.125 to 0.125
- w_rate_up: bfloat16 [128, 1024], P(None, 'tp'), may hold values from -0.5 to 0.5
- rate_base: float32 [1024], P('tp'), may hold values from -10 to 1
- key_scale: float32 [1024], P('tp'), may hold values from 0.25 to 2.5
- key_mix: float32 [1024], P('tp'), may hold values from 0.1 to 0.7
- group_gain: float32 [1024], P('tp'), may hold values from 0.1 to 1.9
- w_out_conv: bfloat16 [1024, 2048], P('tp', 'sp'), may hold values from -0.125 to 0.125
- w_out_state: bfloat16 [1024, 2048], P('tp', 'sp'), may hold values from -0.125 to 0.125
Outputs:
- mixed: bfloat16 [4, 1024, 2048], P('fs', ('sp', 'tp'))
The draws below stay inside these ranges and needn't reach their ends.
All inputs are finite; a program needn't handle non-finite values.
Results may differ from the reference program's by a relative error of at most 0.015.
Values may be sent and summed in bfloat16 or wider, within the bound.
A program may use at most 128 MiB of HBM per device.

```python
import math
import jax
import jax.numpy as jnp
from jax import lax

D = 2048
CONV_CH = 1024
HEADS = 16
HEAD = 64
DECAY_RANK = 128
RATE_RANK = 128
TOK_DEV = 256
STATE_CH = 1024
SERIES_STEPS = 1024
BATCH_SERIES = 4
N_TP = 2


def quick_head_count(key):
    head_count = STATE_CH // HEAD
    order = jax.random.permutation(jax.random.fold_in(key, 101), head_count)
    chosen = order < head_count // 2
    return jnp.repeat(chosen, HEAD)


def draw_decay_base(key, part):
    jitter = jax.random.uniform(jax.random.fold_in(key, 202), (STATE_CH,), jnp.float32, -0.5, 0.5)
    return jnp.where(quick_head_count(key), -3.5 + jitter, -12.0 + jitter)


def draw_rate_base(key, part):
    quick = jax.random.uniform(jax.random.fold_in(key, 303), (STATE_CH,), jnp.float32, -1.0, 1.0)
    slower = jax.random.uniform(jax.random.fold_in(key, 404), (STATE_CH,), jnp.float32, -10.0, -8.0)
    return jnp.where(quick_head_count(key), quick, slower)


def draw_decay_shift(key, part):
    block_count = SERIES_STEPS // TOK_DEV
    levels = jnp.exp(jax.random.uniform(jax.random.fold_in(key, 505), (BATCH_SERIES, block_count, 1, 1), jnp.float32, math.log(3e-06), math.log(6e-05)))
    rough = jnp.exp(jax.random.uniform(jax.random.fold_in(key, 606), (BATCH_SERIES, block_count, TOK_DEV, STATE_CH), jnp.float32, math.log(0.5), math.log(2.0)))
    drift = -(levels * rough).reshape(BATCH_SERIES, SERIES_STEPS, STATE_CH)
    spike_location = jax.random.randint(jax.random.fold_in(key, 707), (BATCH_SERIES, 3), 0, SERIES_STEPS)
    losses = jnp.log(jax.random.uniform(jax.random.fold_in(key, 808), (BATCH_SERIES, 3, STATE_CH), jnp.float32, 0.5, 0.8))
    slot_numbers = jnp.arange(SERIES_STEPS)
    spike_total = (slot_numbers[None, None, :] == spike_location[:, :, None]).astype(jnp.float32)
    return drift + jnp.einsum('sbl,sbc->slc', spike_total, losses)


def level_of(key, dims, split, low, high):
    loudness, own = 1.0, jax.random.fold_in(key, 6)
    for dim, blocks in split:
        heights = jnp.exp(jax.random.uniform(jax.random.fold_in(own, dim), (blocks,), jnp.float32, low / len(split), high / len(split)))
        loudness = loudness * jnp.repeat(heights, dims[dim] // blocks).reshape([-1 if axis == dim else 1 for axis in range(len(dims))])
    return loudness


def scatter_about(rng, extent, width, bound, cuts=(), kind=jnp.bfloat16):
    factor_of = level_of(rng, extent, cuts, -0.22, 0.18) if cuts else 1.0
    entries = jax.random.normal(rng, extent, jnp.float32) * width * factor_of
    return jnp.minimum(jnp.maximum(entries, -bound), bound).astype(kind)


def setup_inputs(seed: int = 0) -> dict:
    streams_of = jax.random.split(jax.random.key(seed), 22)
    return {
        "tokens": scatter_about(streams_of[0], (BATCH_SERIES, SERIES_STEPS, D), 1.0, 6.0, ((0, 4), (1, 8))),
        "norm_gain": jnp.clip(1.0 + 0.18 * jax.random.normal(streams_of[1], (D,), jnp.float32), 0.1, 1.9),
        "w_conv_gate": scatter_about(streams_of[2], (D, CONV_CH), D ** -0.5, 0.125, ((0, 4), (1, 2))),
        "w_conv_in": scatter_about(streams_of[3], (D, CONV_CH), D ** -0.5, 0.125, ((0, 4), (1, 2))),
        "w_conv_value": scatter_about(streams_of[4], (D, CONV_CH), D ** -0.5, 0.125, ((0, 4), (1, 2))),
        "conv_taps": scatter_about(streams_of[5], (3, CONV_CH), 3 ** -0.5, 3.5, ((1, 2),), jnp.float32),
        "w_receptance": scatter_about(streams_of[6], (D, STATE_CH), D ** -0.5, 0.125, ((0, 4), (1, 2))),
        "w_key": scatter_about(streams_of[7], (D, STATE_CH), D ** -0.5, 0.125, ((0, 4), (1, 2))),
        "w_value": scatter_about(streams_of[8], (D, STATE_CH), D ** -0.5, 0.125, ((0, 4), (1, 2))),
        "w_decay_down": scatter_about(streams_of[9], (D, DECAY_RANK), D ** -0.5, 0.125, ((0, 4),)),
        "w_decay_up": scatter_about(streams_of[10], (DECAY_RANK, STATE_CH), (DECAY_RANK // 2) ** -0.5, 0.75, ((1, 2),)),
        "decay_base": draw_decay_base(jax.random.fold_in(streams_of[21], 71), 0),
        "decay_shift": draw_decay_shift(jax.random.fold_in(streams_of[21], 71), 0),
        "w_rate_down": scatter_about(streams_of[13], (D, RATE_RANK), D ** -0.5, 0.125, ((0, 4),)),
        "w_rate_up": scatter_about(streams_of[14], (RATE_RANK, STATE_CH), RATE_RANK ** -0.5, 0.5, ((1, 2),)),
        "rate_base": draw_rate_base(jax.random.fold_in(streams_of[21], 71), 0),
        "key_scale": jnp.clip(jnp.exp(math.log(2.5) - 2.3025851 * jax.random.uniform(streams_of[16], (STATE_CH,), jnp.float32) ** level_of(streams_of[16], (STATE_CH,), ((0, 2),), -0.2, 0.2)), 0.25, 2.5),
        "key_mix": jnp.clip(0.1 + 0.59999999 * jax.random.uniform(streams_of[17], (STATE_CH,), jnp.float32) ** level_of(streams_of[17], (STATE_CH,), ((0, 2),), -0.2, 0.2), 0.1, 0.7),
        "group_gain": jnp.clip(1.0 + 0.18 * jax.random.normal(streams_of[18], (STATE_CH,), jnp.float32), 0.1, 1.9),
        "w_out_conv": scatter_about(streams_of[19], (CONV_CH, D), (CONV_CH + STATE_CH) ** -0.5, 0.125, ((0, 2), (1, 4))),
        "w_out_state": scatter_about(streams_of[20], (STATE_CH, D), (CONV_CH + STATE_CH) ** -0.5, 0.125, ((0, 2), (1, 4))),
    }


highest = lax.Precision.HIGHEST

def normalize_rows(rows_in, norm_gain):
    values = rows_in.astype(jnp.float32)
    scaled = values * lax.rsqrt(lax.optimization_barrier(jnp.mean(values * values, axis=-1, keepdims=True)) + 1e-06)
    return (scaled * norm_gain).astype(jnp.bfloat16)

def project(normed, weight):
    return jnp.dot(normed, weight, preferred_element_type=jnp.float32).astype(jnp.bfloat16)

def recurrence(receptance, decay_mul, key_write, value_vec, erase_vec, replace_vec):

    def advance(memory, inputs_now):
        recv_now, decay_now, key_now, value_now, erase_now, replace_now = inputs_now
        erased = jnp.einsum('hvk,hk->hv', memory, erase_now, precision=highest)
        memory = memory * decay_now[:, None, :] + erased[:, :, None] * replace_now[:, None, :] + value_now[:, :, None] * key_now[:, None, :]
        return (memory, jnp.einsum('hvk,hk->hv', memory, recv_now, precision=highest))
    initial = jnp.zeros((HEADS, HEAD, HEAD), jnp.float32)
    return lax.scan(advance, initial, (receptance, decay_mul, key_write, value_vec, erase_vec, replace_vec))[1]

def merge_outputs(conv_out, state_out, w_out_conv, w_out_state):
    filter_branch_output = CONV_CH // N_TP
    state_part = STATE_CH // N_TP
    combined = jnp.zeros((conv_out.shape[0], w_out_conv.shape[1]), jnp.float32)
    for member in range(N_TP):
        conv_lo = member * filter_branch_output
        state_lo = member * state_part
        partial_sum = jnp.dot(conv_out[:, conv_lo:conv_lo + filter_branch_output], w_out_conv[conv_lo:conv_lo + filter_branch_output], preferred_element_type=jnp.float32) + jnp.dot(state_out[:, state_lo:state_lo + state_part], w_out_state[state_lo:state_lo + state_part], preferred_element_type=jnp.float32)
        rounded = lax.optimization_barrier(partial_sum.astype(jnp.bfloat16))
        combined = combined + rounded.astype(jnp.float32)
    return combined.astype(jnp.bfloat16)

def split_heads(values):
    return values.reshape(values.shape[0], HEADS, HEAD)

def reference(tokens, norm_gain, w_conv_gate, w_conv_in, w_conv_value, conv_taps, w_receptance, w_key, w_value, w_decay_down, w_decay_up, decay_base, decay_shift, w_rate_down, w_rate_up, rate_base, key_scale, key_mix, group_gain, w_out_conv, w_out_state):
    results = []
    for sequence in range(BATCH_SERIES):
        normed = normalize_rows(tokens[sequence], norm_gain)
        conv_gate = project(normed, w_conv_gate)
        filter_source = project(normed, w_conv_in)
        conv_value = project(normed, w_conv_value)
        product_value = filter_source.astype(jnp.float32) * conv_value.astype(jnp.float32)
        padded = jnp.concatenate([jnp.zeros((2, CONV_CH), jnp.float32), product_value], axis=0)
        filtered = conv_taps[0] * padded[:-2] + conv_taps[1] * padded[1:-1] + conv_taps[2] * padded[2:]
        conv_out = (conv_gate.astype(jnp.float32) * filtered).astype(jnp.bfloat16)
        receptance = project(normed, w_receptance)
        key_raw = project(normed, w_key)
        value_raw = project(normed, w_value)
        decay_low = project(normed, w_decay_down)
        rate_low = project(normed, w_rate_down)
        decay_act = jnp.tanh(decay_low.astype(jnp.float32)).astype(jnp.bfloat16)
        decay_pre = decay_base + jnp.dot(decay_act, w_decay_up, preferred_element_type=jnp.float32)
        log_decay = decay_shift[sequence] - jnp.exp(-jax.nn.softplus(-decay_pre) - 0.5)
        learn_rate = jax.nn.sigmoid(rate_base + jnp.dot(rate_low, w_rate_up, preferred_element_type=jnp.float32))
        scaled_key = split_heads(key_raw.astype(jnp.float32) * key_scale)
        erase_dir = scaled_key * lax.rsqrt(lax.optimization_barrier(jnp.sum(scaled_key * scaled_key, axis=-1, keepdims=True)) + 1e-06)
        key_write = key_raw.astype(jnp.float32) * (1.0 + (learn_rate - 1.0) * key_mix)
        readouts = recurrence(split_heads(receptance.astype(jnp.float32)), split_heads(jnp.exp(log_decay)), split_heads(key_write), split_heads(value_raw.astype(jnp.float32)), -erase_dir, erase_dir * split_heads(learn_rate))
        centered = readouts - lax.optimization_barrier(jnp.mean(readouts, axis=-1, keepdims=True))
        variance = lax.optimization_barrier(jnp.mean(centered * centered, axis=-1, keepdims=True))
        normal_heads = (centered * lax.rsqrt(variance + 0.00064)).reshape(SERIES_STEPS, STATE_CH)
        state_out = (normal_heads * group_gain).astype(jnp.bfloat16)
        results.append(merge_outputs(conv_out, state_out, w_out_conv, w_out_state))
    return jnp.stack(results)
```

```python
import functools

import jax
import jax.numpy as jnp
from jax import lax
from jax.experimental import pallas as pl
from jax.experimental.pallas import tpu as pltpu
from jax.sharding import PartitionSpec as P

HEAD = 64
CHUNK = 64
norm_eps = 1e-06
group_eps = 0.00064
f32, bf16 = jnp.float32, jnp.bfloat16

NN = (((1,), (0,)), ((), ()))
NT = (((1,), (1,)), ((), ()))
TN = (((0,), (0,)), ((), ()))
MESH = pl.DeviceIdType.MESH


def dot1(a, b, dims):
    return lax.dot_general(a.astype(bf16), b.astype(bf16), dims, preferred_element_type=f32)


def split2(a):
    high = a.astype(bf16)
    return high, (a - high.astype(f32)).astype(bf16)


def dot3(a, b, dims):
    (ah, al), (bh, bl) = split2(a), split2(b)
    d = functools.partial(lax.dot_general, dimension_numbers=dims, preferred_element_type=f32)
    return d(ah, bh) + (d(ah, bl) + d(al, bh))


def twice(x):
    return jnp.concatenate([x, x], axis=0)


def fold(x):
    half = x.shape[0] // 2
    return x[:half] + x[half:]


def send(src, dst, send_sem, recv_sem, peer):
    return pltpu.make_async_remote_copy(
        src_ref=src, dst_ref=dst, send_sem=send_sem, recv_sem=recv_sem,
        device_id=peer, device_id_type=MESH,
    )


def head_sums(x, low):
    a = jnp.sum(jnp.where(low, x, 0.0), axis=-1, keepdims=True)
    b = jnp.sum(jnp.where(low, 0.0, x), axis=-1, keepdims=True)
    return jnp.where(low, a, b)


def sequence_maps(state_in, shift, decay_up, rate_up, par):
    tokens, width = shift.shape
    rank = decay_up.shape[0]
    decay_base, rate_base, key_scale, key_mix = par
    rounded = state_in.astype(bf16)
    recv, key, val = (rounded[:, i * width : (i + 1) * width].astype(f32) for i in range(3))
    decay_low = rounded[:, 3 * width : 3 * width + rank]
    rate_low = rounded[:, 3 * width + rank :]
    act = jnp.tanh(decay_low.astype(f32)).astype(bf16)
    pre = decay_base + lax.dot_general(act, decay_up, NN, preferred_element_type=f32)
    log_decay = shift - jnp.exp(-0.5) * jax.nn.sigmoid(pre)
    rate = jax.nn.sigmoid(
        rate_base + lax.dot_general(rate_low, rate_up, NN, preferred_element_type=f32)
    )
    low = lax.broadcasted_iota(jnp.int32, (1, width), 1) < HEAD
    scaled = key * key_scale
    erase = scaled * lax.rsqrt(head_sums(scaled * scaled, low) + norm_eps)
    write = key * (1.0 + (rate - 1.0) * key_mix)
    replace = erase * rate
    erase = -erase

    ti = lax.broadcasted_iota(jnp.int32, (tokens, tokens), 0)
    tj = lax.broadcasted_iota(jnp.int32, (tokens, tokens), 1)
    tri = jnp.where(jnp.logical_and(ti >= tj, ti // CHUNK == tj // CHUNK), 1.0, 0.0).astype(bf16)
    first = log_decay.astype(bf16)
    rest = log_decay - first.astype(f32)
    second = rest.astype(bf16)
    third = (rest - second.astype(f32)).astype(bf16)
    sums = lax.dot_general(
        tri, jnp.concatenate([first, second, third], axis=1), NN, preferred_element_type=f32
    )
    incl = sums[:, :width] + (sums[:, width : 2 * width] + sums[:, 2 * width :])
    excl = incl - log_decay

    rows = 2 * CHUNK
    ri = lax.broadcasted_iota(jnp.int32, (rows, rows), 0)
    ci = lax.broadcasted_iota(jnp.int32, (rows, rows), 1)
    same = (ri < CHUNK) == (ci < CHUNK)
    strict = jnp.logical_and(same, ri > ci)
    causal = jnp.logical_and(same, ri >= ci)
    eye = ri == ci
    st = lambda x: jnp.concatenate([jnp.where(low, x, 0.0), jnp.where(low, 0.0, x)], axis=0).astype(bf16)
    two = lambda x: twice(x.astype(bf16))

    chunks = range(tokens // CHUNK)
    sl = [slice(c * CHUNK, (c + 1) * CHUNK) for c in chunks]
    final = [incl[s.stop - 1 : s.stop] for s in sl]
    mid = [incl[s.start + CHUNK // 2 - 1 : s.start + CHUNK // 2] for s in sl]
    up = [jnp.exp(incl[s] - m) for s, m in zip(sl, mid)]
    back = [jnp.exp(m - incl[s]) for s, m in zip(sl, mid)]
    tail = [jnp.exp(f - incl[s]) for s, f in zip(sl, final)]
    left = [
        jnp.concatenate([st(erase[s] * jnp.exp(excl[s] - mid[c])), st(recv[s] * up[c])], axis=0)
        for c, s in enumerate(sl)
    ]
    right = [
        jnp.concatenate([two(replace[s] * back[c]), two(write[s] * back[c])], axis=0)
        for c, s in enumerate(sl)
    ]
    pairs = [dot1(a, b, NT) for a, b in zip(left, right)]
    v = [st(val[s]) for s in sl]
    x = [jnp.where(strict, p[:rows, :rows], 0.0) for p in pairs]
    xb = [a.astype(bf16) for a in x]
    power = [dot1(a, a, NN) for a in xb]
    ekqk = [
        jnp.concatenate(
            [
                jnp.where(strict, p[:rows, rows:], 0.0).astype(bf16),
                jnp.where(causal, p[rows:, rows:], 0.0).astype(bf16),
            ],
            axis=0,
        )
        for p in pairs
    ]
    qr = [jnp.where(causal, p[rows:, :rows], 0.0).astype(bf16) for p in pairs]
    ekv_qkv = [dot1(a, b, NN) for a, b in zip(ekqk, v)]
    inv = [jnp.where(eye, 1.0, a) for a in x]
    reached = 2
    while reached < CHUNK:
        pb = [p.astype(bf16) for p in power]
        ib = [i.astype(bf16) for i in inv]
        if reached * 2 < CHUNK:
            step = [dot1(jnp.concatenate([i, p], axis=0), p, NN) for i, p in zip(ib, pb)]
            inv = [i + s[:rows] for i, s in zip(inv, step)]
            power = [s[rows:] for s in step]
        else:
            step = [dot1(i, p, NN) for i, p in zip(ib, pb)]
            inv = [i + s for i, s in zip(inv, step)]
        reached *= 2
    e_now = [st(erase[s] * jnp.exp(excl[s])) for s in sl]
    solved = [
        dot1(i, jnp.concatenate([e, k[:rows].astype(bf16)], axis=1), NN)
        for i, e, k in zip(inv, e_now, ekv_qkv)
    ]
    seen = [dot1(a, b, NN) for a, b in zip(qr, solved)]
    query, local, step_map, carried = [], [], [], []
    for c, s in enumerate(sl):
        query.append(recv[s] * jnp.exp(incl[s]) + fold(seen[c][:, :width]))
        local.append(fold(seen[c][:, width:] + ekv_qkv[c][rows:]))
    for c, s in enumerate(sl):
        r_end, k_end = replace[s] * tail[c], (write[s] * tail[c]).astype(bf16)
        rh, rl = split2(r_end)
        sh, sl_ = split2(solved[c][:, :width])
        d = functools.partial(lax.dot_general, dimension_numbers=TN, preferred_element_type=f32)
        rh2 = twice(rh)
        moved = d(sh, rh2) + (d(sh, twice(rl)) + d(sl_, rh2))
        step_map.append(jnp.where(eye, jnp.exp(final[c]), 0.0) + jnp.where(same, moved, 0.0))
        added = d(
            jnp.concatenate([solved[c][:, width:].astype(bf16), v[c]], axis=0),
            jnp.concatenate([rh2, twice(k_end)], axis=0),
        )
        carried.append(jnp.where(same, added, 0.0))
    return query, local, step_map, carried


def layer_kernel(
    n_sp, n_fs,
    tok, gain, wr, wk, wv, wdd, wrd, wcg, wci, wcv, woc, wos, shift, wdu, wru,
    decay_base, rate_base, key_scale, key_mix, group_gain, taps,
    out_ref,
    raw, toks, ws, lows, wc, wo, shifts, acc, qm, lm, sm, cm, own_map, maps, state, both,
    halo_out, ext, part, from_pair, sums, from_fs,
    load_sem, tok_send, tok_recv, pair_send, pair_recv, low_send, low_recv, lowp_send, lowp_recv,
    shift_send, shift_recv, z_right, z_left, z_recv, map_send, map_recv, halo_sem, swap_sem,
    fs_send, fs_recv,
):
    n_tp = toks.shape[1]
    rows, dim = tok.shape
    steps, width = shifts.shape[1:]
    depth = ws.shape[1]
    rank = wdd.shape[1]
    share_rows = lows.shape[2]
    sp, fs, tp = lax.axis_index("sp"), lax.axis_index("fs"), lax.axis_index("tp")
    partner = {"tp": 1 - tp}
    if n_fs == 4:
        others = [fs + 1 - 2 * lax.rem(fs, 2), lax.rem(fs + 2, 4), 3 - fs]
    else:
        others = [lax.rem(fs + d, n_fs) for d in range(1, n_fs)]
    share = fs * n_tp + tp
    has_left, has_right = sp > 0, sp < n_sp - 1
    at_end = jnp.logical_or(sp == 0, sp == n_sp - 1)
    mine = lambda: pl.ds(pl.multiple_of(fs * width, width), width)

    def load(k, src, dst):
        return pltpu.make_async_copy(src, dst, load_sem.at[k])

    load_tok = load(0, tok, raw)
    share_of = lambda w: w.at[pl.ds(pl.multiple_of(share * share_rows, share_rows), share_rows), :]
    load_a = [
        load(1, share_of(wdd), lows.at[sp, share, :, pl.ds(0, rank)]),
        load(2, share_of(wrd), lows.at[sp, share, :, pl.ds(rank, rank)]),
    ] + [
        load(3 + i, w.at[:, mine()], ws.at[sp, :, pl.ds(i * width, width)])
        for i, w in enumerate((wr, wk, wv))
    ]
    load_b = [
        load(6 + i, w.at[:, mine()], wc.at[sp, :, pl.ds(i * width, width)])
        for i, w in enumerate((wcg, wci, wcv))
    ]
    load_c = [
        load(9 + i, w.at[mine(), :], wo.at[sp, pl.ds(i * width, width), :])
        for i, w in enumerate((woc, wos))
    ]
    load_shift = load(11, shift.at[:, mine()], shifts.at[fs])
    for copy in [load_tok] + load_a + load_b + load_c + [load_shift]:
        copy.start()

    barrier = pltpu.get_barrier_semaphore()
    peers = [partner] + [{"fs": f} for f in others]
    peers += [{"sp": lax.rem(sp + d, n_sp)} for d in range(1, n_sp)]
    for peer in peers:
        pl.semaphore_signal(barrier, inc=1, device_id=peer, device_id_type=MESH)

    load_tok.wait()
    values = raw[...].astype(f32)
    scaled = values * lax.rsqrt(jnp.mean(values * values, axis=-1, keepdims=True) + norm_eps)
    toks[fs, tp] = (scaled * gain[...]).astype(bf16)
    for copy in load_a:
        copy.wait()
    pl.semaphore_wait(barrier, len(peers))

    def z_slot(stage, j):
        if stage == 0:
            return lows.at[j, share]
        return (ws, wc, wo)[stage - 1].at[j]

    def z_copy(stage, j, to_right):
        sems = z_right if to_right else z_left
        slot = z_slot(stage, j)
        peer = {"sp": sp + 1} if to_right else {"sp": sp - 1}
        return send(slot, slot, sems.at[stage, j], z_recv.at[stage, j], peer)

    def z_start(stage):
        @pl.when(has_right)
        def _():
            z_copy(stage, sp, True).start()

        @pl.when(has_left)
        def _():
            z_copy(stage, sp, False).start()

    def z_forward(stage, k):
        @pl.when(jnp.logical_and(sp >= k, has_right))
        def _():
            z_copy(stage, sp - k, True).wait_recv()
            z_copy(stage, sp - k, True).start()

        @pl.when(jnp.logical_and(sp + k < n_sp, has_left))
        def _():
            z_copy(stage, sp + k, False).wait_recv()
            z_copy(stage, sp + k, False).start()

    def z_take(stage, j):
        @pl.when(at_end)
        def _():
            z_copy(stage, j, True).wait_recv()

    def z_drain(stage):
        for j in range(n_sp):

            @pl.when(jnp.logical_and(sp >= j, has_right))
            def _():
                z_copy(stage, j, True).wait_send()

            @pl.when(jnp.logical_and(sp <= j, has_left))
            def _():
                z_copy(stage, j, False).wait_send()

    turn = 1 - 2 * ((2 * sp) // n_sp)
    nearest = [lax.rem(sp + turn * i + n_sp, n_sp) for i in range(n_sp)]

    z_start(0)
    z_start(1)
    own_tok = toks.at[fs, tp]
    tok_out = [send(own_tok, own_tok, tok_send.at[i], tok_recv.at[fs], {"fs": f}) for i, f in enumerate(others)]
    for copy in tok_out:
        copy.start()
    pair_out = [send(own_tok, own_tok, pair_send.at[0], pair_recv.at[fs], partner)]
    pair_out[0].start()

    def forward_tokens(i):
        there = toks.at[others[i], tp]
        send(there, there, tok_send.at[i], tok_recv.at[others[i]], {"fs": others[i]}).wait_recv()
        copy = send(there, there, pair_send.at[i + 1], pair_recv.at[others[i]], partner)
        copy.start()
        pair_out.append(copy)

    for k in range(1, n_sp):
        z_forward(0, k)
    for i in range(1, n_sp):
        z_take(0, nearest[i])
    own_low = lows.at[:, share]
    low_out = [send(own_low, own_low, low_send.at[i], low_recv.at[fs], {"fs": f}) for i, f in enumerate(others)]
    lowp_out = [send(own_low, own_low, lowp_send.at[0], lowp_recv.at[fs], partner)]
    for copy in low_out + lowp_out:
        copy.start()
    z_forward(1, 1)
    for copy in load_b:
        copy.wait()
    shift_out = [
        send(
            shift.at[:, pl.ds(pl.multiple_of(f * width, width), width)], shifts.at[fs],
            shift_send.at[i], shift_recv.at[fs], {"fs": f},
        )
        for i, f in enumerate(others)
    ]
    for copy in shift_out:
        copy.start()
    for i in range(n_fs - 1):
        forward_tokens(i)
        if i + 2 < n_sp:
            z_forward(1, i + 2)
    for k in range(n_fs + 1, n_sp):
        z_forward(1, k)
    z_start(2)
    for i, f in enumerate(others):
        there = lows.at[:, f * n_tp + tp]
        send(there, there, low_send.at[i], low_recv.at[f], {"fs": f}).wait_recv()
        copy = send(there, there, lowp_send.at[i + 1], lowp_recv.at[f], partner)
        copy.start()
        lowp_out.append(copy)
    for f in [fs] + others:
        there = toks.at[f, 1 - tp]
        send(there, there, pair_send.at[0], pair_recv.at[f], partner).wait_recv()
    for f in [fs] + others:
        there = lows.at[:, f * n_tp + 1 - tp]
        send(there, there, lowp_send.at[0], lowp_recv.at[f], partner).wait_recv()

    def project(weights, column, take):
        wide = weights.shape[-1]
        if depth % 128 == 0:
            for i, j in enumerate(nearest):
                if i and take is not None:
                    z_take(take, j)
                cut = toks[:, :, :, pl.ds(pl.multiple_of(j * depth, depth), depth)]
                block = weights[j].reshape(depth, wide)
                term = lax.dot_general(
                    cut.reshape(n_fs * steps, depth), block, NN, preferred_element_type=f32
                ).reshape(n_fs, steps, wide)
                if i:
                    term = acc[:, :, pl.ds(column, wide)] + term
                acc[:, :, pl.ds(column, wide)] = term
        else:
            for i in range(1, n_sp):
                if take is not None:
                    z_take(take, nearest[i])
            whole = weights[...].reshape(dim, wide)
            acc[:, :, pl.ds(column, wide)] = lax.dot_general(
                toks[...].reshape(n_fs * steps, dim), whole, NN, preferred_element_type=f32
            ).reshape(n_fs, steps, wide)

    project(lows, 3 * width, None)
    project(ws, 0, 1)
    load_shift.wait()
    for i, f in enumerate(others):
        send(shifts.at[f], shifts.at[f], shift_send.at[i], shift_recv.at[f], {"fs": f}).wait_recv()

    par = [p[:, mine()] for p in (decay_base, rate_base, key_scale, key_mix)]
    decay_up, rate_up = wdu[:, mine()], wru[:, mine()]
    n_chunk = steps // CHUNK

    def one_sequence(f, carry):
        query, local, step_map, carried = sequence_maps(acc[f], shifts[f], decay_up, rate_up, par)
        for c in range(n_chunk):
            qm[f, pl.ds(c * CHUNK, CHUNK)] = query[c]
            lm[f, pl.ds(c * CHUNK, CHUNK)] = local[c]
            sm[f, c] = step_map[c]
            cm[f, c] = carried[c]
        k = f + 1

        @pl.when(jnp.logical_and(sp >= k, has_right))
        def _():
            z_copy(2, sp - k, True).wait_recv()
            z_copy(2, sp - k, True).start()

        @pl.when(jnp.logical_and(sp + k < n_sp, has_left))
        def _():
            z_copy(2, sp + k, False).wait_recv()
            z_copy(2, sp + k, False).start()

        return carry

    lax.fori_loop(0, n_fs, one_sequence, 0)
    for k in range(n_fs + 1, n_sp):
        z_forward(2, k)
    for copy in load_c:
        copy.wait()
    z_start(3)

    total = [jnp.concatenate([sm[f, 0], cm[f, 0]], axis=0) for f in range(n_fs)]
    square = 2 * CHUNK
    for c in range(1, n_chunk):
        cut = pl.ds(c * CHUNK, CHUNK)
        for f in range(n_fs):
            seen = dot1(qm[f, cut], total[f], NT)
            qm[f, cut] = seen[:, :square]
            lm[f, cut] = lm[f, cut] + seen[:, square:]
        total = [dot3(total[f], sm[f, c], NN) for f in range(n_fs)]
        total = [
            jnp.concatenate([t[:square], t[square:] + cm[f, c]], axis=0) for f, t in enumerate(total)
        ]
    for f in range(n_fs):
        own_map[f, 0] = fold(total[f][:square]).astype(bf16)
        own_map[f, 1] = fold(total[f][square:]).astype(bf16)

    def map_copy(k):
        return send(own_map, maps.at[sp], map_send.at[k], map_recv.at[sp], {"sp": sp + k})

    for k in range(1, n_sp):

        @pl.when(sp + k < n_sp)
        def _():
            map_copy(k).start()

    project(wc, 0, 2)
    for k in range(1, n_sp):
        z_forward(3, k)
    edge = ext.shape[1] - steps
    for f in range(n_fs):
        source = acc[f, :, pl.ds(width, width)].astype(bf16).astype(f32)
        value = acc[f, :, pl.ds(2 * width, width)].astype(bf16).astype(f32)
        product = source * value
        ext[f, pl.ds(edge, steps)] = product
        halo_out[f] = product[steps - edge :]
    halo_in = from_halo = halo_out.at[pl.ds(n_fs, n_fs)]
    halo = send(
        halo_out.at[pl.ds(0, n_fs)], halo_in, halo_sem.at[0], halo_sem.at[1], {"sp": sp + 1}
    )

    @pl.when(has_right)
    def _():
        halo.start()

    @pl.when(has_left)
    def _():
        send(from_halo, from_halo, halo_sem.at[0], halo_sem.at[1], {"sp": sp - 1}).wait_recv()
        ext[:, pl.ds(0, edge)] = halo_out[pl.ds(n_fs, n_fs)]

    @pl.when(sp == 0)
    def _():
        ext[:, pl.ds(0, edge)] = jnp.zeros((n_fs, edge, width), f32)

    tap = taps[:, mine()]
    for f in range(n_fs):
        filtered = (
            tap[0:1] * ext[f, pl.ds(edge - 2, steps)]
            + tap[1:2] * ext[f, pl.ds(edge - 1, steps)]
            + tap[2:3] * ext[f, pl.ds(edge, steps)]
        )
        gate = acc[f, :, pl.ds(0, width)].astype(bf16).astype(f32)
        both[f, :, pl.ds(0, width)] = (gate * filtered).astype(bf16)

    wi = lax.broadcasted_iota(jnp.int32, (width, width), 0)
    wj = lax.broadcasted_iota(jnp.int32, (width, width), 1)
    same = (wi < HEAD) == (wj < HEAD)
    widen = lambda x: jnp.where(same, twice(x.astype(f32)), 0.0)

    @pl.when(sp == 0)
    def _():
        state[...] = jnp.zeros(state.shape, f32)

    for hop in range(n_sp - 1):

        @pl.when(hop < sp)
        def _():
            slot = maps.at[hop]
            send(slot, slot, map_send.at[0], map_recv.at[hop], {"sp": sp - 1}).wait_recv()
            if hop == 0:
                for f in range(n_fs):
                    state[f] = widen(maps[hop, f, 1])
            else:
                new = [dot1x(state[f], widen(maps[hop, f, 0])) for f in range(n_fs)]
                for f in range(n_fs):
                    state[f] = new[f] + widen(maps[hop, f, 1])

    low = lax.broadcasted_iota(jnp.int32, (1, width), 1) < HEAD
    gains = group_gain[:, mine()]
    for f in range(n_fs):
        read = lm[f] + dot1(qm[f], state[f], NT)
        centered = read - head_sums(read, low) * (1.0 / HEAD)
        var = head_sums(centered * centered, low) * (1.0 / HEAD)
        both[f, :, pl.ds(width, width)] = (centered * lax.rsqrt(var + group_eps) * gains).astype(bf16)

    cols = wo.shape[2]
    n_blk, wide = part.shape[0], part.shape[-1]
    per = wide // cols
    if per > 1:
        for i in range(1, n_sp):
            z_take(3, nearest[i])
    blocks = nearest if per == 1 else list(range(n_blk))
    lanes = [pl.ds(pl.multiple_of(j * wide, 128), wide) for j in blocks]
    swaps, fs_out = [], []
    for i, j in enumerate(blocks):
        if per == 1:
            if i:
                z_take(3, j)
            weights = wo[j]
        else:
            weights = jnp.concatenate([wo[j * per + q] for q in range(per)], axis=1)
        term = lax.dot_general(
            both[...].reshape(n_fs * steps, both.shape[-1]), weights, NN, preferred_element_type=f32
        )
        part[i] = term.astype(bf16).reshape(n_fs, n_tp, rows, wide)
        swap = send(part.at[i, :, 1 - tp], from_pair.at[i], swap_sem.at[0, i], swap_sem.at[1, i], partner)
        swap.start()
        swaps.append(swap)
        swap.wait_recv()
        for q, f in enumerate(others + [fs]):
            total_f = part[i, f, tp].astype(f32) + from_pair[i, f].astype(f32)
            sums[i, q] = total_f.astype(bf16)
            if q < n_fs - 1:
                copy = send(sums.at[i, q], from_fs.at[i, q], fs_send.at[i, q], fs_recv.at[i, q], {"fs": f})
                copy.start()
                fs_out.append(copy)
    for i in range(n_blk):
        result = sums[i, n_fs - 1].astype(f32)
        for q in range(n_fs - 1):
            fs_out[i * (n_fs - 1) + q].wait_recv()
            result = result + from_fs[i, q].astype(f32)
        out_ref[:, lanes[i]] = result.astype(bf16)

    for copy in tok_out + pair_out + low_out + lowp_out + shift_out + swaps + fs_out:
        copy.wait_send()
    for stage in range(4):
        z_drain(stage)
    for k in range(1, n_sp):

        @pl.when(sp + k < n_sp)
        def _():
            map_copy(k).wait_send()

    @pl.when(has_right)
    def _():
        halo.wait_send()


def dot1x(a, b):
    return dot3(a, b, NN)


def body(
    tokens, norm_gain, w_conv_gate, w_conv_in, w_conv_value, conv_taps, w_receptance, w_key,
    w_value, w_decay_down, w_decay_up, decay_base, decay_shift, w_rate_down, w_rate_up,
    rate_base, key_scale, key_mix, group_gain, w_out_conv, w_out_state,
):
    n_fs, n_sp, n_tp = (lax.axis_size(a) for a in ("fs", "sp", "tp"))
    rows, dim = tokens.shape[1:]
    steps = decay_shift.shape[1]
    depth, width = w_key.shape[0], w_key.shape[1] // n_fs
    rank = w_decay_down.shape[1]
    cols = w_out_conv.shape[1]
    n_share = n_fs * n_tp
    wide = max(cols, dim // 4)
    n_blk = dim // wide
    n_chunk = steps // CHUNK
    any_, vmem = pl.BlockSpec(memory_space=pl.ANY), pl.BlockSpec(memory_space=pltpu.VMEM)
    dma = lambda *n: pltpu.SemaphoreType.DMA(n)
    row = lambda p: p.reshape(1, -1)
    edge = 8
    mixed = pl.pallas_call(
        functools.partial(layer_kernel, n_sp, n_fs),
        in_specs=[any_, vmem] + [any_] * 11 + [vmem] * 8,
        out_specs=vmem,
        out_shape=jax.ShapeDtypeStruct((rows, dim), bf16),
        scratch_shapes=[
            pltpu.VMEM((rows, dim), bf16),
            pltpu.VMEM((n_fs, n_tp, rows, dim), bf16),
            pltpu.VMEM((n_sp, depth, 3 * width), bf16),
            pltpu.VMEM((n_sp, n_share, depth // n_share, 2 * rank), bf16),
            pltpu.VMEM((n_sp, depth, 3 * width), bf16),
            pltpu.VMEM((n_sp, 2 * width, cols), bf16),
            pltpu.VMEM((n_fs, steps, width), f32),
            pltpu.VMEM((n_fs, steps, 3 * width + 2 * rank), f32),
            pltpu.VMEM((n_fs, steps, width), f32),
            pltpu.VMEM((n_fs, steps, width), f32),
            pltpu.VMEM((n_fs, n_chunk, width, width), f32),
            pltpu.VMEM((n_fs, n_chunk, width, width), f32),
            pltpu.VMEM((n_fs, 2, HEAD, width), bf16),
            pltpu.VMEM((n_sp, n_fs, 2, HEAD, width), bf16),
            pltpu.VMEM((n_fs, width, width), f32),
            pltpu.VMEM((n_fs, steps, 2 * width), bf16),
            pltpu.VMEM((2 * n_fs, edge, width), f32),
            pltpu.VMEM((n_fs, edge + steps, width), f32),
            pltpu.VMEM((n_blk, n_fs, n_tp, rows, wide), bf16),
            pltpu.VMEM((n_blk, n_fs, rows, wide), bf16),
            pltpu.VMEM((n_blk, n_fs, rows, wide), bf16),
            pltpu.VMEM((n_blk, n_fs - 1, rows, wide), bf16),
            dma(12), dma(n_fs), dma(n_fs), dma(n_fs), dma(n_fs), dma(n_fs), dma(n_fs), dma(n_fs),
            dma(n_fs), dma(n_fs), dma(n_fs), dma(4, n_sp), dma(4, n_sp), dma(4, n_sp), dma(n_sp),
            dma(n_sp), dma(2), dma(2, n_blk), dma(n_blk, n_fs), dma(n_blk, n_fs),
        ],
        compiler_params=pltpu.CompilerParams(collective_id=0, has_side_effects=True),
    )(
        tokens[0], row(norm_gain), w_receptance, w_key, w_value, w_decay_down, w_rate_down,
        w_conv_gate, w_conv_in, w_conv_value, w_out_conv, w_out_state, decay_shift[0],
        w_decay_up, w_rate_up, row(decay_base), row(rate_base), row(key_scale), row(key_mix),
        row(group_gain), conv_taps,
    )
    return mixed[None]


def solution(mesh):
    in_specs = (
        P("fs", ("sp", "tp"), None), P(), P("sp", "tp"), P("sp", "tp"), P("sp", "tp"),
        P(None, "tp"), P("sp", "tp"), P("sp", "tp"), P("sp", "tp"), P("sp", None), P(None, "tp"),
        P("tp"), P("fs", "sp", "tp"), P("sp", None), P(None, "tp"), P("tp"), P("tp"), P("tp"),
        P("tp"), P("tp", "sp"), P("tp", "sp"),
    )
    out_specs = P("fs", ("sp", "tp"), None)
    return jax.shard_map(body, mesh=mesh, in_specs=in_specs, out_specs=out_specs, check_vma=False)
```

```python
import functools

import jax
import jax.numpy as jnp
from jax import lax
from jax.experimental import pallas as pl
from jax.experimental.pallas import tpu as pltpu
from jax.sharding import PartitionSpec as P

HEAD = 64
CHUNK = 64
norm_eps = 1e-06
group_eps = 0.00064
f32, bf16 = jnp.float32, jnp.bfloat16

NN = (((1,), (0,)), ((), ()))
NT = (((1,), (1,)), ((), ()))
TN = (((0,), (0,)), ((), ()))
MESH = pl.DeviceIdType.MESH


def dot1(a, b, dims):
    return lax.dot_general(a.astype(bf16), b.astype(bf16), dims, preferred_element_type=f32)


def split2(a):
    high = a.astype(bf16)
    return high, (a - high.astype(f32)).astype(bf16)


def dot3(a, b, dims):
    (ah, al), (bh, bl) = split2(a), split2(b)
    d = functools.partial(lax.dot_general, dimension_numbers=dims, preferred_element_type=f32)
    return d(ah, bh) + (d(ah, bl) + d(al, bh))


def twice(x):
    return jnp.concatenate([x, x], axis=0)


def fold(x):
    half = x.shape[0] // 2
    return x[:half] + x[half:]


def send(src, dst, send_sem, recv_sem, peer):
    return pltpu.make_async_remote_copy(
        src_ref=src, dst_ref=dst, send_sem=send_sem, recv_sem=recv_sem,
        device_id=peer, device_id_type=MESH,
    )


def head_sums(x, low):
    a = jnp.sum(jnp.where(low, x, 0.0), axis=-1, keepdims=True)
    b = jnp.sum(jnp.where(low, 0.0, x), axis=-1, keepdims=True)
    return jnp.where(low, a, b)


def sequence_maps(state_in, shift, decay_up, rate_up, par):
    tokens, width = shift.shape
    rank = decay_up.shape[0]
    decay_base, rate_base, key_scale, key_mix = par
    rounded = state_in.astype(bf16)
    recv, key, val = (rounded[:, i * width : (i + 1) * width].astype(f32) for i in range(3))
    decay_low = rounded[:, 3 * width : 3 * width + rank]
    rate_low = rounded[:, 3 * width + rank :]
    act = jnp.tanh(decay_low.astype(f32)).astype(bf16)
    pre = decay_base + lax.dot_general(act, decay_up, NN, preferred_element_type=f32)
    log_decay = shift - jnp.exp(-0.5) * jax.nn.sigmoid(pre)
    rate = jax.nn.sigmoid(
        rate_base + lax.dot_general(rate_low, rate_up, NN, preferred_element_type=f32)
    )
    low = lax.broadcasted_iota(jnp.int32, (1, width), 1) < HEAD
    scaled = key * key_scale
    erase = scaled * lax.rsqrt(head_sums(scaled * scaled, low) + norm_eps)
    write = key * (1.0 + (rate - 1.0) * key_mix)
    replace = erase * rate
    erase = -erase

    ti = lax.broadcasted_iota(jnp.int32, (tokens, tokens), 0)
    tj = lax.broadcasted_iota(jnp.int32, (tokens, tokens), 1)
    tri = jnp.where(jnp.logical_and(ti >= tj, ti // CHUNK == tj // CHUNK), 1.0, 0.0).astype(bf16)
    first = log_decay.astype(bf16)
    rest = log_decay - first.astype(f32)
    second = rest.astype(bf16)
    third = (rest - second.astype(f32)).astype(bf16)
    sums = lax.dot_general(
        tri, jnp.concatenate([first, second, third], axis=1), NN, preferred_element_type=f32
    )
    incl = sums[:, :width] + (sums[:, width : 2 * width] + sums[:, 2 * width :])
    excl = incl - log_decay

    rows = 2 * CHUNK
    ri = lax.broadcasted_iota(jnp.int32, (rows, rows), 0)
    ci = lax.broadcasted_iota(jnp.int32, (rows, rows), 1)
    same = (ri < CHUNK) == (ci < CHUNK)
    strict = jnp.logical_and(same, ri > ci)
    causal = jnp.logical_and(same, ri >= ci)
    eye = ri == ci
    st = lambda x: jnp.concatenate([jnp.where(low, x, 0.0), jnp.where(low, 0.0, x)], axis=0).astype(bf16)
    two = lambda x: twice(x.astype(bf16))

    chunks = range(tokens // CHUNK)
    sl = [slice(c * CHUNK, (c + 1) * CHUNK) for c in chunks]
    final = [incl[s.stop - 1 : s.stop] for s in sl]
    mid = [incl[s.start + CHUNK // 2 - 1 : s.start + CHUNK // 2] for s in sl]
    up = [jnp.exp(incl[s] - m) for s, m in zip(sl, mid)]
    back = [jnp.exp(m - incl[s]) for s, m in zip(sl, mid)]
    tail = [jnp.exp(f - incl[s]) for s, f in zip(sl, final)]
    left = [
        jnp.concatenate([st(erase[s] * jnp.exp(excl[s] - mid[c])), st(recv[s] * up[c])], axis=0)
        for c, s in enumerate(sl)
    ]
    right = [
        jnp.concatenate([two(replace[s] * back[c]), two(write[s] * back[c])], axis=0)
        for c, s in enumerate(sl)
    ]
    pairs = [dot1(a, b, NT) for a, b in zip(left, right)]
    v = [st(val[s]) for s in sl]
    x = [jnp.where(strict, p[:rows, :rows], 0.0) for p in pairs]
    xb = [a.astype(bf16) for a in x]
    power = [dot1(a, a, NN) for a in xb]
    ekqk = [
        jnp.concatenate(
            [
                jnp.where(strict, p[:rows, rows:], 0.0).astype(bf16),
                jnp.where(causal, p[rows:, rows:], 0.0).astype(bf16),
            ],
            axis=0,
        )
        for p in pairs
    ]
    qr = [jnp.where(causal, p[rows:, :rows], 0.0).astype(bf16) for p in pairs]
    ekv_qkv = [dot1(a, b, NN) for a, b in zip(ekqk, v)]
    inv = [jnp.where(eye, 1.0, a) for a in x]
    reached = 2
    while reached < CHUNK:
        pb = [p.astype(bf16) for p in power]
        ib = [i.astype(bf16) for i in inv]
        if reached * 2 < CHUNK:
            step = [dot1(jnp.concatenate([i, p], axis=0), p, NN) for i, p in zip(ib, pb)]
            inv = [i + s[:rows] for i, s in zip(inv, step)]
            power = [s[rows:] for s in step]
        else:
            step = [dot1(i, p, NN) for i, p in zip(ib, pb)]
            inv = [i + s for i, s in zip(inv, step)]
        reached *= 2
    e_now = [st(erase[s] * jnp.exp(excl[s])) for s in sl]
    solved = [
        dot1(i, jnp.concatenate([e, k[:rows].astype(bf16)], axis=1), NN)
        for i, e, k in zip(inv, e_now, ekv_qkv)
    ]
    seen = [dot1(a, b, NN) for a, b in zip(qr, solved)]
    query, local, step_map, carried = [], [], [], []
    for c, s in enumerate(sl):
        query.append(recv[s] * jnp.exp(incl[s]) + fold(seen[c][:, :width]))
        local.append(fold(seen[c][:, width:] + ekv_qkv[c][rows:]))
    for c, s in enumerate(sl):
        r_end, k_end = replace[s] * tail[c], (write[s] * tail[c]).astype(bf16)
        rh, rl = split2(r_end)
        sh, sl_ = split2(solved[c][:, :width])
        d = functools.partial(lax.dot_general, dimension_numbers=TN, preferred_element_type=f32)
        rh2 = twice(rh)
        moved = d(sh, rh2) + (d(sh, twice(rl)) + d(sl_, rh2))
        step_map.append(jnp.where(eye, jnp.exp(final[c]), 0.0) + jnp.where(same, moved, 0.0))
        added = d(
            jnp.concatenate([solved[c][:, width:].astype(bf16), v[c]], axis=0),
            jnp.concatenate([rh2, twice(k_end)], axis=0),
        )
        carried.append(jnp.where(same, added, 0.0))
    return query, local, step_map, carried


def layer_kernel(
    n_sp, n_fs,
    tok, gain, wr, wk, wv, wdd, wrd, wcg, wci, wcv, woc, wos, shift, wdu, wru,
    decay_base, rate_base, key_scale, key_mix, group_gain, taps,
    out_ref,
    raw, toks, ws, lows, wc, wo, shifts, acc, qm, lm, sm, cm, tm, state_out, state_in, state, both,
    halo_buf, ext, part, from_pair, sums, from_x, from_y, relay, relayed,
    load_sem, tok_sem, tok_recv, pair_send, pair_recv, low_send, low_recv, lowp_send, lowp_recv,
    shift_send, shift_recv, z_right, z_left, z_recv, state_sem, halo_sem, swap_sem,
    fs_send, fs_recv,
):
    n_tp = toks.shape[1]
    rows, dim = tok.shape
    steps, width = shifts.shape[1:]
    depth = ws.shape[1]
    rank = wdd.shape[1]
    share_rows = lows.shape[2]
    sp, fs, tp = lax.axis_index("sp"), lax.axis_index("fs"), lax.axis_index("tp")
    partner = {"tp": 1 - tp}
    if n_fs == 4:
        others = [fs + 1 - 2 * lax.rem(fs, 2), lax.rem(fs + 2, 4), 3 - fs]
    else:
        others = [lax.rem(fs + d, n_fs) for d in range(1, n_fs)]
    share = fs * n_tp + tp
    has_left, has_right = sp > 0, sp < n_sp - 1
    at_end = jnp.logical_or(sp == 0, sp == n_sp - 1)
    mine = lambda: pl.ds(pl.multiple_of(fs * width, width), width)

    def load(k, src, dst):
        return pltpu.make_async_copy(src, dst, load_sem.at[k])

    load_tok = load(0, tok, raw)
    share_of = lambda w: w.at[pl.ds(pl.multiple_of(share * share_rows, share_rows), share_rows), :]
    load_a = [
        load(1, share_of(wdd), lows.at[sp, share, :, pl.ds(0, rank)]),
        load(2, share_of(wrd), lows.at[sp, share, :, pl.ds(rank, rank)]),
    ] + [
        load(3 + i, w.at[:, mine()], ws.at[sp, :, pl.ds(i * width, width)])
        for i, w in enumerate((wr, wk, wv))
    ]
    load_b = [
        load(6 + i, w.at[:, mine()], wc.at[sp, :, pl.ds(i * width, width)])
        for i, w in enumerate((wcg, wci, wcv))
    ]
    load_c = [
        load(9 + i, w.at[mine(), :], wo.at[sp, pl.ds(i * width, width), :])
        for i, w in enumerate((woc, wos))
    ]
    load_shift = load(11, shift.at[:, mine()], shifts.at[fs])
    for copy in [load_tok] + load_a + load_b + load_c + [load_shift]:
        copy.start()

    barrier = pltpu.get_barrier_semaphore()
    peers = [partner] + [{"fs": f} for f in others]
    for peer in peers:
        pl.semaphore_signal(barrier, inc=1, device_id=peer, device_id_type=MESH)

    @pl.when(has_left)
    def _():
        pl.semaphore_signal(barrier, inc=1, device_id={"sp": sp - 1}, device_id_type=MESH)

    @pl.when(has_right)
    def _():
        pl.semaphore_signal(barrier, inc=1, device_id={"sp": sp + 1}, device_id_type=MESH)

    load_tok.wait()
    values = raw[...].astype(f32)
    scaled = values * lax.rsqrt(jnp.mean(values * values, axis=-1, keepdims=True) + norm_eps)
    toks[fs, tp] = (scaled * gain[...]).astype(bf16)
    for copy in load_a + load_b + load_c:
        copy.wait()
    pl.semaphore_wait(barrier, len(peers) + has_left.astype(jnp.int32) + has_right.astype(jnp.int32))

    cols = wo.shape[2]
    n_blk, wide = part.shape[0], part.shape[-1]
    row_pieces = max(1, depth // 128)
    n_piece = (1, row_pieces, row_pieces, max(1, cols // wide))

    def z_slot(stage, j, q):
        if stage == 0:
            return lows.at[j, share]
        if stage < 3:
            size = depth // row_pieces
            return (ws, wc)[stage - 1].at[j, pl.ds(q * size, size)]
        return wo.at[j, :, pl.ds(q * wide, wide)] if n_piece[3] > 1 else wo.at[j]

    def z_copy(stage, j, q, to_right):
        sems = z_right if to_right else z_left
        slot = z_slot(stage, j, q)
        peer = {"sp": sp + 1} if to_right else {"sp": sp - 1}
        return send(slot, slot, sems.at[stage, j, q], z_recv.at[stage, j, q], peer)

    def z_own(stage, to_right, when, pieces=None):
        @pl.when(jnp.logical_and(when, has_right if to_right else has_left))
        def _():
            for q in range(n_piece[stage]) if pieces is None else pieces:
                z_copy(stage, sp, q, to_right).start()

    def z_hop(stage, k, to_right, when=True, pieces=None, wait=True, start=True):
        ahead = sp if to_right else n_sp - 1 - sp
        here = jnp.logical_and(when, has_right if to_right else has_left)
        j = sp - k if to_right else sp + k
        pieces = range(n_piece[stage]) if pieces is None else pieces

        if k:

            @pl.when(jnp.logical_and(here, ahead >= k))
            def _():
                for q in pieces:
                    if wait:
                        z_copy(stage, j, q, to_right).wait_recv()
                    if start:
                        z_copy(stage, j, q, to_right).start()

        if start and n_piece[stage] - 1 in pieces and 0 < stage < 3:
            z_own(stage + 1, to_right, jnp.logical_and(when, ahead == k))

    def z_both(stage, k, pieces=None, **how):
        z_hop(stage, k, True, True, pieces, **how)
        z_hop(stage, k, False, True, pieces, **how)

    right_short = 2 * sp < n_sp

    def z_short(stage, k):
        z_hop(stage, k, True, right_short)
        z_hop(stage, k, False, jnp.logical_not(right_short))

    def z_long(stage, k):
        z_hop(stage, k, True, jnp.logical_not(right_short))
        z_hop(stage, k, False, right_short)

    def z_take(stage, j, pieces=None):
        @pl.when(at_end)
        def _():
            for q in range(n_piece[stage]) if pieces is None else pieces:
                z_copy(stage, j, q, True).wait_recv()

    def z_drain(stage):
        for j in range(n_sp):

            @pl.when(jnp.logical_and(sp >= j, has_right))
            def _():
                for q in range(n_piece[stage]):
                    z_copy(stage, j, q, True).wait_send()

            @pl.when(jnp.logical_and(sp <= j, has_left))
            def _():
                for q in range(n_piece[stage]):
                    z_copy(stage, j, q, False).wait_send()

    turn = 1 - 2 * ((2 * sp) // n_sp)
    nearest = [lax.rem(sp + turn * i + n_sp, n_sp) for i in range(n_sp)]

    last = row_pieces - 1
    batch = [range(0, (last + 1) // 2), range((last + 1) // 2, last + 1)]

    def own_state(pieces):
        z_own(1, True, True, pieces)
        z_own(1, False, True, pieces)

    z_own(0, True, True)
    z_own(0, False, True)
    own_state(range(0, last // 2))

    half = rows // 2
    tok_slot = lambda f, t, h: toks.at[f, t, pl.ds(h * half, half)]
    tok_out, pair_out = [], []

    def tok_send_to(f, h, peer, sem):
        slot = tok_slot(f, tp, h)
        copy = send(slot, slot, tok_sem.at[sem], tok_recv.at[f, h], {"fs": peer})
        copy.start()
        tok_out.append(copy)

    def tok_wait(f, h):
        slot = tok_slot(f, tp, h)
        send(slot, slot, tok_sem.at[0], tok_recv.at[f, h], {"fs": f}).wait_recv()

    def tok_pair(f, h, sem):
        slot = tok_slot(f, tp, h)
        copy = send(slot, slot, pair_send.at[sem], pair_recv.at[f, h], partner)
        copy.start()
        pair_out.append(copy)

    near_x, near_y, far = others
    tok_send_to(fs, 0, near_x, 0)
    tok_send_to(fs, 1, near_y, 1)
    tok_send_to(fs, 1, near_x, 2)
    tok_send_to(fs, 0, near_y, 3)
    tok_pair(fs, 0, 0)
    tok_pair(fs, 1, 1)

    z_both(0, 1)
    own_state(range(last // 2, last))
    for k in range(2, n_sp):
        z_both(0, k)
    own_state(range(last, last + 1))
    for stage in (1, 2):
        z_hop(stage, 0, True)
        z_hop(stage, 0, False)
    z_both(1, 1, batch[0])
    tok_wait(near_x, 0)
    tok_send_to(near_x, 0, near_y, 4)
    tok_wait(near_y, 1)
    tok_send_to(near_y, 1, near_x, 5)
    tok_pair(near_x, 0, 2)
    tok_pair(near_y, 1, 3)
    for i in range(1, n_sp):
        z_take(0, nearest[i])
    own_low = lows.at[:, share]
    low_out = [send(own_low, own_low, low_send.at[i], low_recv.at[fs], {"fs": f}) for i, f in enumerate(others)]
    lowp_out = [send(own_low, own_low, lowp_send.at[0], lowp_recv.at[fs], partner)]
    for copy in low_out + lowp_out:
        copy.start()
    shift_out = [
        send(
            shift.at[:, pl.ds(pl.multiple_of(f * width, width), width)], shifts.at[fs],
            shift_send.at[i], shift_recv.at[fs], {"fs": f},
        )
        for i, f in enumerate(others)
    ]
    for copy in shift_out:
        copy.start()
    z_both(1, 1, batch[1])
    tok_wait(near_x, 1)
    tok_pair(near_x, 1, 4)
    tok_wait(near_y, 0)
    tok_pair(near_y, 0, 5)
    z_both(1, 2, batch[0])
    tok_wait(far, 0)
    tok_pair(far, 0, 6)
    tok_wait(far, 1)
    tok_pair(far, 1, 7)
    z_both(1, 2, batch[1])
    for k in range(3, n_sp):
        z_both(1, k)
    z_short(2, 1)
    for f in [fs] + others:
        for h in range(2):
            slot = tok_slot(f, 1 - tp, h)
            send(slot, slot, pair_send.at[0], pair_recv.at[f, h], partner).wait_recv()

    def take_low():
        for i, f in enumerate(others):
            there = lows.at[:, f * n_tp + tp]
            send(there, there, low_send.at[i], low_recv.at[f], {"fs": f}).wait_recv()
            copy = send(there, there, lowp_send.at[i + 1], lowp_recv.at[f], partner)
            copy.start()
            lowp_out.append(copy)
        for f in [fs] + others:
            there = lows.at[:, f * n_tp + 1 - tp]
            send(there, there, lowp_send.at[0], lowp_recv.at[f], partner).wait_recv()

    def project(weights, column, take, order):
        wide = weights.shape[-1]
        if depth % 128 == 0:
            for i in order:
                j = nearest[i]
                if i and take is not None:
                    z_take(take, j)
                cut = toks[:, :, :, pl.ds(pl.multiple_of(j * depth, depth), depth)]
                block = weights[j].reshape(depth, wide)
                term = lax.dot_general(
                    cut.reshape(n_fs * steps, depth), block, NN, preferred_element_type=f32
                ).reshape(n_fs, steps, wide)
                if i:
                    term = acc[:, :, pl.ds(column, wide)] + term
                acc[:, :, pl.ds(column, wide)] = term
        elif n_sp - 1 in order:
            for i in range(1, n_sp):
                if take is not None:
                    z_take(take, nearest[i])
            whole = weights[...].reshape(dim, wide)
            acc[:, :, pl.ds(column, wide)] = lax.dot_general(
                toks[...].reshape(n_fs * steps, dim), whole, NN, preferred_element_type=f32
            ).reshape(n_fs, steps, wide)

    project(ws, 0, 1, range(n_sp - 1))
    take_low()
    project(lows, 3 * width, None, range(n_sp))
    project(ws, 0, 1, [n_sp - 1])
    load_shift.wait()
    for i, f in enumerate(others):
        send(shifts.at[f], shifts.at[f], shift_send.at[i], shift_recv.at[f], {"fs": f}).wait_recv()

    par = [p[:, mine()] for p in (decay_base, rate_base, key_scale, key_mix)]
    decay_up, rate_up = wdu[:, mine()], wru[:, mine()]
    n_chunk = steps // CHUNK

    def one_sequence(f, carry):
        query, local, step_map, carried = sequence_maps(acc[f], shifts[f], decay_up, rate_up, par)
        for c in range(n_chunk):
            qm[f, pl.ds(c * CHUNK, CHUNK)] = query[c]
            lm[f, pl.ds(c * CHUNK, CHUNK)] = local[c]
            sm[f, c] = step_map[c]
            cm[f, c] = carried[c]

        @pl.when(f == n_fs // 2 - 1)
        def _():
            z_long(2, 1)

        return carry

    lax.fori_loop(0, n_fs, one_sequence, 0)

    total = [jnp.concatenate([sm[f, 0], cm[f, 0]], axis=0) for f in range(n_fs)]
    square = 2 * CHUNK
    for c in range(1, n_chunk):
        cut = pl.ds(c * CHUNK, CHUNK)
        for f in range(n_fs):
            seen = dot1(qm[f, cut], total[f], NT)
            qm[f, cut] = seen[:, :square]
            lm[f, cut] = lm[f, cut] + seen[:, square:]
        total = [dot3(total[f], sm[f, c], NN) for f in range(n_fs)]
        total = [
            jnp.concatenate([t[:square], t[square:] + cm[f, c]], axis=0) for f, t in enumerate(total)
        ]
    for f in range(n_fs):
        tm[f] = total[f]
    state_copy = send(state_out, state_in, state_sem.at[0], state_sem.at[1], {"sp": sp + 1})

    @pl.when(sp == 0)
    def _():
        state[...] = jnp.zeros(state.shape, f32)
        for f in range(n_fs):
            state_out[f] = fold(tm[f, pl.ds(square, square)]).astype(bf16)

        @pl.when(has_right)
        def _():
            state_copy.start()

    edge = ext.shape[1] - steps
    halo = send(
        halo_buf.at[0], halo_buf.at[1], halo_sem.at[0], halo_sem.at[1], {"sp": sp + 1}
    )

    def convolve():
        project(wc, 0, 2, range(n_sp))
        for f in range(n_fs):
            source = acc[f, :, pl.ds(width, width)].astype(bf16).astype(f32)
            value = acc[f, :, pl.ds(2 * width, width)].astype(bf16).astype(f32)
            product = source * value
            ext[f, pl.ds(edge, steps)] = product
            halo_buf[0, f] = product[steps - edge :]

        @pl.when(has_right)
        def _():
            halo.start()

    farthest = n_sp - 2
    for k in range(2, farthest):
        z_both(2, k)
    if farthest > 1:
        z_both(2, farthest, start=False)

    @pl.when(jnp.logical_not(at_end))
    def _():
        convolve()

    if farthest > 1:
        z_both(2, farthest, batch[0], wait=False)
    wi = lax.broadcasted_iota(jnp.int32, (width, width), 0)
    wj = lax.broadcasted_iota(jnp.int32, (width, width), 1)
    same = (wi < HEAD) == (wj < HEAD)

    @pl.when(has_left)
    def _():
        state_copy.wait_recv()
        for f in range(n_fs):
            state[f] = jnp.where(same, twice(state_in[f].astype(f32)), 0.0)

    @pl.when(jnp.logical_and(has_left, has_right))
    def _():
        new = [dot3(state[f], tm[f, pl.ds(0, square)], NN) for f in range(n_fs)]
        for f in range(n_fs):
            state_out[f] = fold(new[f] + tm[f, pl.ds(square, square)]).astype(bf16)
        state_copy.start()

    if farthest > 1:
        z_both(2, farthest, batch[1], wait=False)
    z_short(3, 1)
    low = lax.broadcasted_iota(jnp.int32, (1, width), 1) < HEAD
    gains = group_gain[:, mine()]
    for f in range(n_fs):
        read = lm[f] + dot1(qm[f], state[f], NT)
        centered = read - head_sums(read, low) * (1.0 / HEAD)
        var = head_sums(centered * centered, low) * (1.0 / HEAD)
        both[f, :, pl.ds(width, width)] = (centered * lax.rsqrt(var + group_eps) * gains).astype(bf16)

    @pl.when(at_end)
    def _():
        convolve()

    z_long(3, 1)
    for k in range(2, n_sp):
        z_both(3, k)

    @pl.when(has_left)
    def _():
        halo.wait_recv()
        ext[:, pl.ds(0, edge)] = halo_buf[1]

    @pl.when(sp == 0)
    def _():
        ext[:, pl.ds(0, edge)] = jnp.zeros((n_fs, edge, width), f32)

    tap = taps[:, mine()]
    for f in range(n_fs):
        filtered = (
            tap[0:1] * ext[f, pl.ds(edge - 2, steps)]
            + tap[1:2] * ext[f, pl.ds(edge - 1, steps)]
            + tap[2:3] * ext[f, pl.ds(edge, steps)]
        )
        gate = acc[f, :, pl.ds(0, width)].astype(bf16).astype(f32)
        both[f, :, pl.ds(0, width)] = (gate * filtered).astype(bf16)

    per, n_cut, lag = max(1, wide // cols), n_piece[3], 2
    if n_cut == 1:
        for i in range(1, n_sp):
            z_take(3, nearest[i])
    upper, lower = pl.ds(0, half), pl.ds(half, half)
    order = [near_x, far, near_y, fs]
    swaps, first_out, second_out, lanes = [], [], [], []

    def first_step(i):
        over_x = send(
            sums.at[i, pl.ds(0, 2), upper], from_x.at[i], fs_send.at[i, 0], fs_recv.at[i, 0],
            {"fs": near_x},
        )
        over_y = send(
            sums.at[i, pl.ds(1, 2), lower], from_y.at[i], fs_send.at[i, 1], fs_recv.at[i, 1],
            {"fs": near_y},
        )
        over_x.start()
        over_y.start()
        first_out.append((over_x, over_y))

    def second_step(i):
        over_x, over_y = first_out[i]
        over_x.wait_recv()
        relay[i, 0] = (sums[i, 2, upper].astype(f32) + from_x[i, 1].astype(f32)).astype(bf16)
        to_y = send(relay.at[i, 0], relayed.at[i, 0], fs_send.at[i, 2], fs_recv.at[i, 2], {"fs": near_y})
        to_y.start()
        over_y.wait_recv()
        relay[i, 1] = (sums[i, 0, lower].astype(f32) + from_y[i, 0].astype(f32)).astype(bf16)
        to_x = send(relay.at[i, 1], relayed.at[i, 1], fs_send.at[i, 3], fs_recv.at[i, 3], {"fs": near_x})
        to_x.start()
        second_out.append((to_y, to_x))

    def finish_block(i):
        to_y, to_x = second_out[i]
        to_y.wait_recv()
        to_x.wait_recv()
        for cut_rows, h, got in ((upper, 0, from_x[i, 0]), (lower, 1, from_y[i, 1])):
            result = sums[i, 3, cut_rows].astype(f32) + got.astype(f32) + relayed[i, h].astype(f32)
            out_ref[cut_rows, lanes[i]] = result.astype(bf16)

    for i in range(n_blk):
        if per == 1:
            j, q = nearest[i // n_cut], i % n_cut
            if i >= n_cut and n_cut > 1:
                z_take(3, j, [q])
            weights = wo[j, :, pl.ds(q * wide, wide)]
            lanes.append(pl.ds(pl.multiple_of(j * cols + q * wide, 128), wide))
        else:
            weights = jnp.concatenate([wo[i * per + q] for q in range(per)], axis=1)
            lanes.append(pl.ds(i * wide, wide))
        term = lax.dot_general(
            both[...].reshape(n_fs * steps, both.shape[-1]), weights, NN, preferred_element_type=f32
        )
        part[i] = term.astype(bf16).reshape(n_fs, n_tp, rows, wide)
        swap = send(part.at[i, :, 1 - tp], from_pair.at[i], swap_sem.at[0, i], swap_sem.at[1, i], partner)
        swap.start()
        swaps.append(swap)
        if i >= lag:
            second_step(i - lag)
        swap.wait_recv()
        for q, f in enumerate(order):
            sums[i, q] = (part[i, f, tp].astype(f32) + from_pair[i, f].astype(f32)).astype(bf16)
        first_step(i)
        if i >= 2 * lag:
            finish_block(i - 2 * lag)
    for i in range(max(0, n_blk - lag), n_blk):
        second_step(i)
    for i in range(max(0, n_blk - 2 * lag), n_blk):
        finish_block(i)

    for copy in tok_out + pair_out + low_out + lowp_out + shift_out + swaps:
        copy.wait_send()
    for pair in first_out + second_out:
        for copy in pair:
            copy.wait_send()
    for stage in range(4):
        z_drain(stage)

    @pl.when(has_right)
    def _():
        state_copy.wait_send()
        halo.wait_send()


def body(
    tokens, norm_gain, w_conv_gate, w_conv_in, w_conv_value, conv_taps, w_receptance, w_key,
    w_value, w_decay_down, w_decay_up, decay_base, decay_shift, w_rate_down, w_rate_up,
    rate_base, key_scale, key_mix, group_gain, w_out_conv, w_out_state,
):
    n_fs, n_sp, n_tp = (lax.axis_size(a) for a in ("fs", "sp", "tp"))
    rows, dim = tokens.shape[1:]
    steps = decay_shift.shape[1]
    depth, width = w_key.shape[0], w_key.shape[1] // n_fs
    rank = w_decay_down.shape[1]
    cols = w_out_conv.shape[1]
    n_share = n_fs * n_tp
    wide = dim // 8
    n_blk = dim // wide
    n_chunk = steps // CHUNK
    n_piece = max(1, depth // 128)
    any_, vmem = pl.BlockSpec(memory_space=pl.ANY), pl.BlockSpec(memory_space=pltpu.VMEM)
    dma = lambda *n: pltpu.SemaphoreType.DMA(n)
    row = lambda p: p.reshape(1, -1)
    edge = 8
    mixed = pl.pallas_call(
        functools.partial(layer_kernel, n_sp, n_fs),
        in_specs=[any_, vmem] + [any_] * 11 + [vmem] * 8,
        out_specs=vmem,
        out_shape=jax.ShapeDtypeStruct((rows, dim), bf16),
        scratch_shapes=[
            pltpu.VMEM((rows, dim), bf16),
            pltpu.VMEM((n_fs, n_tp, rows, dim), bf16),
            pltpu.VMEM((n_sp, depth, 3 * width), bf16),
            pltpu.VMEM((n_sp, n_share, depth // n_share, 2 * rank), bf16),
            pltpu.VMEM((n_sp, depth, 3 * width), bf16),
            pltpu.VMEM((n_sp, 2 * width, cols), bf16),
            pltpu.VMEM((n_fs, steps, width), f32),
            pltpu.VMEM((n_fs, steps, 3 * width + 2 * rank), f32),
            pltpu.VMEM((n_fs, steps, width), f32),
            pltpu.VMEM((n_fs, steps, width), f32),
            pltpu.VMEM((n_fs, n_chunk, width, width), f32),
            pltpu.VMEM((n_fs, n_chunk, width, width), f32),
            pltpu.VMEM((n_fs, 2 * width, width), f32),
            pltpu.VMEM((n_fs, HEAD, width), bf16),
            pltpu.VMEM((n_fs, HEAD, width), bf16),
            pltpu.VMEM((n_fs, width, width), f32),
            pltpu.VMEM((n_fs, steps, 2 * width), bf16),
            pltpu.VMEM((2, n_fs, edge, width), f32),
            pltpu.VMEM((n_fs, edge + steps, width), f32),
            pltpu.VMEM((n_blk, n_fs, n_tp, rows, wide), bf16),
            pltpu.VMEM((n_blk, n_fs, rows, wide), bf16),
            pltpu.VMEM((n_blk, n_fs, rows, wide), bf16),
            pltpu.VMEM((n_blk, 2, rows // 2, wide), bf16),
            pltpu.VMEM((n_blk, 2, rows // 2, wide), bf16),
            pltpu.VMEM((n_blk, 2, rows // 2, wide), bf16),
            pltpu.VMEM((n_blk, 2, rows // 2, wide), bf16),
            dma(12), dma(6), dma(n_fs, 2), dma(2 * n_fs), dma(n_fs, 2), dma(n_fs), dma(n_fs), dma(n_fs),
            dma(n_fs), dma(n_fs), dma(n_fs), dma(4, n_sp, n_piece), dma(4, n_sp, n_piece),
            dma(4, n_sp, n_piece), dma(2),
            dma(2), dma(2, n_blk), dma(n_blk, 4), dma(n_blk, 4),
        ],
        compiler_params=pltpu.CompilerParams(collective_id=0, has_side_effects=True),
    )(
        tokens[0], row(norm_gain), w_receptance, w_key, w_value, w_decay_down, w_rate_down,
        w_conv_gate, w_conv_in, w_conv_value, w_out_conv, w_out_state, decay_shift[0],
        w_decay_up, w_rate_up, row(decay_base), row(rate_base), row(key_scale), row(key_mix),
        row(group_gain), conv_taps,
    )
    return mixed[None]


def solution(mesh):
    in_specs = (
        P("fs", ("sp", "tp"), None), P(), P("sp", "tp"), P("sp", "tp"), P("sp", "tp"),
        P(None, "tp"), P("sp", "tp"), P("sp", "tp"), P("sp", "tp"), P("sp", None), P(None, "tp"),
        P("tp"), P("fs", "sp", "tp"), P("sp", None), P(None, "tp"), P("tp"), P("tp"), P("tp"),
        P("tp"), P("tp", "sp"), P("tp", "sp"),
    )
    out_specs = P("fs", ("sp", "tp"), None)
    return jax.shard_map(body, mesh=mesh, in_specs=in_specs, out_specs=out_specs, check_vma=False)
```
